32 devices in a mesh: ep: 8 (over z, y), tp: 4 (over x, core).
Axes of the slice: x: 2, y: 2, z: 4, core: 2. Of those that a mesh axis runs over, the one named last changes fastest.
Arguments:
- query_latent: bfloat16 [1024, 768], P('ep'), may hold values from -6 to 6
- keyval_latent: bfloat16 [1024, 512], P('ep'), may hold values from -6 to 6
- rotary_key: bfloat16 [1024, 32], P('ep'), may hold values from -6 to 6
- query_gain: float32 [768], replicated, may hold values from 0.3 to 48
- keyval_gain: float32 [512], replicated, may hold values from 0.1 to 1.9
- query_weight: bfloat16 [768, 1536], P(None, 'tp'), may hold values from -0.21875 to 0.21875
- keyval_weight: bfloat16 [512, 2048], P(None, 'tp'), may hold values from -0.25 to 0.25
- output_weight: bfloat16 [1024, 2048], P('tp'), may hold values from -0.1875 to 0.1875
- output_gain: float32 [2048], replicated, may hold values from 0.1 to 1.9
- second_rows: bfloat16 [1024, 2048], P('ep'), may hold values from -6 to 6
- second_gain: float32 [2048], replicated, may hold values from 0.1 to 1.9
- route_ids: int32 [1024, 4], P('ep'), may hold values from 0 to 7, all different within a row; in each aligned block of 128 rows (0 to 127, 128 to 255, ...) at most 128 rows name the same one
- route_weights: float32 [1024, 4], P('ep'), may hold values from 0.1 to 1
- gate_weight: bfloat16 [8, 2048, 1024], P('ep', None, 'tp'), may hold values from -0.125 to 0.125
- up_weight: bfloat16 [8, 2048, 1024], P('ep', None, 'tp'), may hold values from -0.125 to 0.125
- down_weight: bfloat16 [8, 1024, 2048], P('ep', 'tp'), may hold values from -0.1875 to 0.1875
- shared_gate: bfloat16 [2048, 512], P(None, 'tp'), may hold values from -0.125 to 0.125
- shared_up: bfloat16 [2048, 512], P(None, 'tp'), may hold values from -0.125 to 0.125
- shared_down: bfloat16 [512, 2048], P('tp'), may hold values from -0.25 to 0.25
Outputs:
- mixed: bfloat16 [1024, 2048], P(('ep', 'tp'))
- expert_mix: bfloat16 [1024, 2048], P('ep', 'tp')
The draws below stay inside these ranges and needn't reach their ends.
Inputs may be any that keep to these rules, and one draw needn't show every extreme that they name: `route_ids`: each row names 4 different experts. Among the rows of one index of ep (aligned blocks of 128 rows) no expert is named more than 128 times, a bound that some expert reaches in some blocks.
All inputs are finite; a program needn't handle non-finite values.
Results may differ from the reference program's by a relative error of at most 0.023.
The reference program's roundings to bfloat16 on the way count: a program that leaves them out, or rounds other values in their place, can miss the bound.
Values may be sent and summed in bfloat16 or wider, within the bound.
A program may use at most 128 MiB of HBM per device.

```python
import math
import jax
import jax.numpy as jnp
import numpy as np
from jax import lax

D = 2048
HEADS = 16
NOPE = 64
ROPE = 32
VDIM = 64
QLAT = 768
KVLAT = 512
FE = 1024
FS = 512
TOP = 4
TOKB = 128
SEQ = 1024
TOKENS_B = 1024
EXPERTS = 8
CAP = 128
N_EP = 8
N_TP = 4


def draw_query_gain(key, part):
    return jax.random.uniform(key, (QLAT,), jnp.float32, 0.3, 1.7)


def levels(key, extent, cuts, low, largest):
    def one(axis_at, blocks):
        draws = jax.random.uniform(jax.random.fold_in(jax.random.fold_in(key, 6), axis_at), (blocks,), jnp.float32, low / len(cuts), largest / len(cuts))
        return jnp.repeat(jnp.exp(draws), extent[axis_at] // blocks).reshape((-1,) + (1,) * (len(extent) - axis_at - 1))

    loudness = one(*cuts[0])
    for cut in cuts[1:]:
        loudness = loudness * one(*cut)
    return loudness


def assign_block(stream_key, own, number, rows, count, top, bound, lean):
    ranking = jax.random.permutation(stream_key, count)
    packed, common = shares(count, rows * top, bound, lean, True), shares(count, rows * top, bound, lean, False)
    places = jnp.arange(count)

    def named(tallies, turn):
        used = int((tallies > 0).sum())
        fixed = max(1, used // 4)
        moved = fixed + (places - fixed + turn * (used - fixed)) % max(1, count - fixed)
        return jnp.zeros((count,), jnp.int32).at[ranking[jnp.where(places < fixed, places, moved)]].set(jnp.asarray(tallies, jnp.int32))

    tallies = jnp.where(number % 4 == 0, named(packed, number // 4), named(common, number - number // 4 - 1))
    mixed = jax.random.permutation(jax.random.fold_in(own, 3), count)
    source_of, taker = mixed[0:count // 2 * 2:2], mixed[1:count // 2 * 2:2]
    margin = jnp.minimum(tallies[source_of] - 1, bound - tallies[taker]) // 2
    margin = jnp.where((source_of == ranking[0]) | (taker == ranking[0]) | (tallies[taker] == 0), 0, jnp.maximum(margin, 0))
    moved = jax.random.randint(jax.random.fold_in(own, 4), (count // 2,), 0, 1 << 20) % (margin + 1)
    tallies = tallies.at[source_of].add(-moved).at[taker].add(moved)
    labels = jnp.searchsorted(jnp.cumsum(tallies), jnp.arange(rows * top), side="right").astype(jnp.int32)
    table = labels.reshape(top, rows).T
    table = table[jax.random.permutation(jax.random.fold_in(own, 1), rows)]
    turn = jax.random.randint(jax.random.fold_in(own, 2), (rows, 1), 0, top)
    return jnp.take_along_axis(table, (jnp.arange(top)[None, :] + turn) % top, axis=1)


def shares(amount, total, reach, skew, full):
    portions = [(1 << 20) // math.isqrt(grade ** skew) + 1 for grade in range(1, amount + 1)]
    largest = reach if full else min(reach, max(-(-total // amount), total * portions[0] // sum(portions)))
    least = 1 if total - largest >= amount - 1 else 0
    holding, spare = [largest] + [least] * (amount - 1), total - largest - least * (amount - 1)
    while spare > 0:
        movable = [i for i in range(1, amount) if holding[i] < largest] or [i for i in range(1, amount) if holding[i] < reach]
        mass, left = sum([portions[i] for i in movable]), spare
        for i in movable:
            more = min(reach - holding[i], max(1, left * portions[i] // mass), spare)
            holding[i] = holding[i] + more
            spare = spare - more
    return np.array(holding)


def scatter_about(own_key, dims, spread, limit, shards=(), held_as=jnp.bfloat16):
    values = spread * jax.random.normal(own_key, dims, jnp.float32)
    if shards:
        values = values * levels(own_key, dims, shards, -0.22, 0.18)
    return jnp.clip(values, -limit, limit).astype(held_as)


def setup_inputs(seed: int = 0) -> dict:
    seeds = jax.random.split(jax.random.key(seed), 20)
    query_latent = scatter_about(seeds[0], (SEQ, QLAT), 1.0, 6.0, ((0, 8),))
    keyval_latent = scatter_about(seeds[1], (SEQ, KVLAT), 1.0, 6.0, ((0, 8),))
    rotary_key = scatter_about(seeds[2], (SEQ, ROPE), 1.0, 6.0, ((0, 8),))
    query_gain = draw_query_gain(jax.random.fold_in(seeds[19], 71), 0)
    keyval_gain = jnp.clip(1.0 + 0.18 * jax.random.normal(seeds[4], (KVLAT,), jnp.float32), 0.1, 1.9)
    query_weight = scatter_about(seeds[5], (QLAT, HEADS * (NOPE + ROPE)), QLAT ** -0.5, 0.21875, ((1, 4),))
    keyval_weight = scatter_about(seeds[6], (KVLAT, HEADS * (NOPE + VDIM)), KVLAT ** -0.5, 0.25, ((1, 4),))
    output_weight = scatter_about(seeds[7], (HEADS * VDIM, D), (HEADS * VDIM) ** -0.5, 0.1875, ((0, 4),))
    output_gain = jnp.clip(1.0 + 0.18 * jax.random.normal(seeds[8], (D,), jnp.float32), 0.1, 1.9)
    second_rows = scatter_about(seeds[9], (TOKENS_B, D), 1.0, 6.0, ((0, 8),))
    second_gain = jnp.clip(1.0 + 0.18 * jax.random.normal(seeds[10], (D,), jnp.float32), 0.1, 1.9)
    route_ids_keys = jax.random.split(jax.random.fold_in(seeds[11], 1), TOKENS_B // TOKB)
    route_ids_turns = jax.random.permutation(jax.random.fold_in(seeds[11], 3), TOKENS_B // TOKB)
    route_ids = jax.vmap(lambda own, number: assign_block(jax.random.fold_in(seeds[11], 2), own, number, TOKB, EXPERTS, TOP, CAP, 1))(route_ids_keys, route_ids_turns).reshape((TOKENS_B, TOP))
    route_weights = jnp.clip(0.1 + 0.9 * jax.random.uniform(seeds[12], (TOKENS_B, TOP), jnp.float32) ** levels(seeds[12], (TOKENS_B, TOP), ((0, 8),), -0.2, 0.2), 0.1, 1.0)
    gate_weight = scatter_about(seeds[13], (EXPERTS, D, FE), D ** -0.5, 0.125, ((0, 8), (2, 4)))
    up_weight = scatter_about(seeds[14], (EXPERTS, D, FE), D ** -0.5, 0.125, ((0, 8), (2, 4)))
    down_weight = scatter_about(seeds[15], (EXPERTS, FE, D), FE ** -0.5, 0.1875, ((0, 8), (1, 4)))
    shared_gate = scatter_about(seeds[16], (D, FS), D ** -0.5, 0.125, ((1, 4),))
    shared_up = scatter_about(seeds[17], (D, FS), D ** -0.5, 0.125, ((1, 4),))
    shared_down = scatter_about(seeds[18], (FS, D), FS ** -0.5, 0.25, ((0, 4),))
    return {"query_latent": query_latent, "keyval_latent": keyval_latent, "rotary_key": rotary_key, "query_gain": query_gain, "keyval_gain": keyval_gain, "query_weight": query_weight, "keyval_weight": keyval_weight, "output_weight": output_weight, "output_gain": output_gain, "second_rows": second_rows, "second_gain": second_gain, "route_ids": route_ids, "route_weights": route_weights, "gate_weight": gate_weight, "up_weight": up_weight, "down_weight": down_weight, "shared_gate": shared_gate, "shared_up": shared_up, "shared_down": shared_down}


EPS = 1e-06
ROPE_BASE = 10000.0

def rms_scale(values, gain_vec):
    widened = values.astype(jnp.float32)
    normed = widened * lax.rsqrt(lax.optimization_barrier(jnp.mean(widened * widened, -1, keepdims=True)) + EPS)
    return (normed * gain_vec.astype(jnp.float32)).astype(jnp.bfloat16)

def rotate(values, positions):
    half_width = values.shape[-1] // 2
    inverse = 1.0 / ROPE_BASE ** (jnp.arange(half_width, dtype=jnp.float32) * 2.0 / (2 * half_width))
    angles = positions[:, None] * inverse[None, :]
    cosine = jnp.cos(angles)
    sine_vals = jnp.sin(angles)
    if values.ndim == 3:
        cosine = cosine[:, None, :]
        sine_vals = sine_vals[:, None, :]
    first_half = values[..., :half_width]
    second = values[..., half_width:]
    return jnp.concatenate([first_half * cosine - second * sine_vals, first_half * sine_vals + second * cosine], -1)

def round_trip(values):
    return lax.optimization_barrier(values.astype(jnp.bfloat16)).astype(jnp.float32)

def attention_part(query_latent, keyval_latent, rotary_key, query_gain, keyval_gain, query_weight, keyval_weight, output_weight, output_gain):
    positions = jnp.arange(SEQ, dtype=jnp.float32)
    queries = jnp.dot(rms_scale(query_latent, query_gain), query_weight, preferred_element_type=jnp.float32).reshape(SEQ, HEADS, NOPE + ROPE)
    queries = jnp.concatenate([queries[..., :NOPE], rotate(queries[..., NOPE:], positions)], -1).astype(jnp.bfloat16)
    keyvals = jnp.dot(rms_scale(keyval_latent, keyval_gain), keyval_weight, preferred_element_type=jnp.float32).astype(jnp.bfloat16)
    keyvals = keyvals.reshape(SEQ, HEADS, NOPE + VDIM)
    key_rot = rotate(rotary_key.astype(jnp.float32), positions).astype(jnp.bfloat16)
    key_plain = keyvals[..., :NOPE].astype(jnp.float32)
    values_all = keyvals[..., NOPE:].astype(jnp.float32)
    key_rot_wide = key_rot.astype(jnp.float32)
    score_scale = (NOPE + ROPE) ** (-0.5)
    block_rows = math.gcd(SEQ, 512)
    blocks = queries.reshape(SEQ // block_rows, block_rows, HEADS, NOPE + ROPE)

    def attend(query_block):
        query_wide = query_block.astype(jnp.float32)
        scores = jnp.einsum('qhd,khd->hqk', query_wide[..., :NOPE], key_plain)
        scores = (scores + jnp.einsum('qhr,kr->hqk', query_wide[..., NOPE:], key_rot_wide)) * score_scale
        top_score = lax.optimization_barrier(jnp.max(scores, -1, keepdims=True))
        exponent = jnp.exp(scores - top_score)
        denominator = lax.optimization_barrier(jnp.sum(exponent, -1))
        summed = jnp.einsum('hqk,khe->qhe', round_trip(exponent), values_all)
        return (summed / denominator.T[..., None]).astype(jnp.bfloat16)
    attended = lax.map(attend, blocks).reshape(SEQ, HEADS * VDIM)
    group_cols = HEADS * VDIM // N_TP
    mixture = jnp.zeros((SEQ, D), jnp.float32)
    for group_idx in range(N_TP):
        lower = group_idx * group_cols
        partial_value = jnp.dot(attended[:, lower:lower + group_cols], output_weight[lower:lower + group_cols], preferred_element_type=jnp.float32)
        mixture = mixture + round_trip(partial_value)
    return rms_scale(mixture, output_gain)

def grouped_down(hidden, down_mat, width):
    group_width = width // N_TP
    output = jnp.zeros((hidden.shape[0], down_mat.shape[1]), jnp.float32)
    for group_idx in range(N_TP):
        lower = group_idx * group_width
        partial_value = jnp.dot(hidden[:, lower:lower + group_width], down_mat[lower:lower + group_width], preferred_element_type=jnp.float32)
        output = output + round_trip(partial_value)
    return output

def expert_part(second_rows, second_gain, route_ids, route_weights, gate_weight, up_weight, down_weight, shared_gate, shared_up, shared_down):
    normed = rms_scale(second_rows, second_gain)
    padded = jnp.concatenate([normed, jnp.zeros((1, D), jnp.bfloat16)], 0)
    block_ids = route_ids.reshape(N_EP, TOKB * TOP)
    onehot = (block_ids[:, :, None] == jnp.arange(EXPERTS, dtype=jnp.int32)[None, None, :]).astype(jnp.int32)
    slot_rank = lax.optimization_barrier(jnp.sum((jnp.cumsum(onehot, 1) - 1) * onehot, 2))
    owners = (jnp.arange(N_EP * TOKB * TOP, dtype=jnp.int32) // TOP).reshape(N_EP, TOKB * TOP)
    sources = jnp.arange(N_EP, dtype=jnp.int32)[:, None]
    target = ((block_ids * N_EP + sources) * CAP + slot_rank).reshape(-1)
    slot_table = jnp.full((EXPERTS * N_EP * CAP,), N_EP * TOKB, jnp.int32).at[target].set(owners.reshape(-1))

    def run_expert(operands):
        gate_mat, up_mat, down_mat, rows_index = operands
        inputs = padded[rows_index]
        gate_act = jnp.dot(inputs, gate_mat, preferred_element_type=jnp.float32)
        up_act = jnp.dot(inputs, up_mat, preferred_element_type=jnp.float32)
        hidden = (jax.nn.silu(gate_act) * up_act).astype(jnp.bfloat16)
        return grouped_down(hidden, down_mat, FE).astype(jnp.bfloat16)
    expert_out = lax.map(run_expert, (gate_weight, up_weight, down_weight, slot_table.reshape(EXPERTS, N_EP * CAP)))
    expert_out = expert_out.reshape(EXPERTS * N_EP * CAP, D)
    picked = expert_out[target].astype(jnp.float32).reshape(N_EP * TOKB, TOP, D)
    routed = lax.optimization_barrier(jnp.sum(picked * route_weights.astype(jnp.float32)[:, :, None], 1))
    shared_hidden = (jax.nn.silu(jnp.dot(normed, shared_gate, preferred_element_type=jnp.float32)) * jnp.dot(normed, shared_up, preferred_element_type=jnp.float32)).astype(jnp.bfloat16)
    shared_out = grouped_down(shared_hidden, shared_down, FS)
    return (routed + shared_out).astype(jnp.bfloat16)

def reference(query_latent, keyval_latent, rotary_key, query_gain, keyval_gain, query_weight, keyval_weight, output_weight, output_gain, second_rows, second_gain, route_ids, route_weights, gate_weight, up_weight, down_weight, shared_gate, shared_up, shared_down):
    mixed = attention_part(query_latent, keyval_latent, rotary_key, query_gain, keyval_gain, query_weight, keyval_weight, output_weight, output_gain)
    expert_mix = expert_part(second_rows, second_gain, route_ids, route_weights, gate_weight, up_weight, down_weight, shared_gate, shared_up, shared_down)
    return (mixed, expert_mix)
```

```python
import functools
import math

import jax
import jax.numpy as jnp
from jax import lax
from jax.experimental import pallas as pl
from jax.experimental.pallas import tpu as pltpu
from jax.sharding import PartitionSpec as P

NOPE = 64
ROPE = 32
VDIM = 64


EPS = 1e-06
ROPE_BASE = 10000.0


def rms_scale(values, gain_vec):
    widened = values.astype(jnp.float32)
    normed = widened * lax.rsqrt(jnp.mean(widened * widened, -1, keepdims=True) + EPS)
    return (normed * gain_vec).astype(jnp.bfloat16)


def rotate(values, positions):
    half_width = values.shape[-1] // 2
    inverse = 1.0 / ROPE_BASE ** (
        jnp.arange(half_width, dtype=jnp.float32) * 2.0 / (2 * half_width)
    )
    angles = positions[:, None] * inverse[None, :]
    cosine = jnp.cos(angles)
    sine_vals = jnp.sin(angles)
    if values.ndim == 3:
        cosine = cosine[:, None, :]
        sine_vals = sine_vals[:, None, :]
    first_half = values[..., :half_width]
    second = values[..., half_width:]
    return jnp.concatenate(
        [first_half * cosine - second * sine_vals, first_half * sine_vals + second * cosine], -1
    )


def per_device_slots(
    query_latent,
    keyval_latent,
    rotary_key,
    query_gain,
    keyval_gain,
    query_weight,
    keyval_weight,
    output_weight,
    output_gain,
    second_rows,
    second_gain,
    route_ids,
    route_weights,
    gate_weight,
    up_weight,
    down_weight,
    shared_gate,
    shared_up,
    shared_down,
):
    first_rows = query_latent.shape[0]
    tp_count = lax.axis_size("tp")
    ep_count = lax.axis_size("ep")
    head_count = query_weight.shape[1] // (NOPE + ROPE)
    positions = (lax.axis_index("ep") * first_rows).astype(jnp.float32) + jnp.arange(
        first_rows, dtype=jnp.float32
    )
    queries = jnp.dot(
        rms_scale(query_latent, query_gain), query_weight, preferred_element_type=jnp.float32
    ).reshape(first_rows, head_count, NOPE + ROPE)
    queries = jnp.concatenate(
        [queries[..., :NOPE], rotate(queries[..., NOPE:], positions)], -1
    ).astype(jnp.bfloat16)
    query_plain = queries[..., :NOPE]
    query_turned = queries[..., NOPE:]
    kv_normed = rms_scale(keyval_latent, keyval_gain)
    key_rot = rotate(rotary_key.astype(jnp.float32), positions).astype(jnp.bfloat16)
    score_scale = (NOPE + ROPE) ** (-0.5)

    def attend(carried, pieces):
        highest, denominator, accumulated = carried
        keyval_piece, rot_piece = pieces
        key_count = keyval_piece.shape[0]
        keyval_heads = keyval_piece.reshape(key_count, head_count, NOPE + VDIM)
        scores = jnp.einsum(
            "qhd,khd->hqk",
            query_plain,
            keyval_heads[..., :NOPE],
            preferred_element_type=jnp.float32,
        )
        scores = (
            scores
            + jnp.einsum("qhr,kr->hqk", query_turned, rot_piece, preferred_element_type=jnp.float32)
        ) * score_scale
        new_high = jnp.maximum(highest, jnp.max(scores, -1))
        exponent = jnp.exp(scores - new_high[..., None])
        rescale = jnp.exp(highest - new_high)
        denominator = denominator * rescale + jnp.sum(exponent, -1)
        update = jnp.einsum(
            "hqk,khe->qhe",
            exponent.astype(jnp.bfloat16),
            keyval_heads[..., NOPE:],
            preferred_element_type=jnp.float32,
        )
        accumulated = accumulated * rescale.T[..., None] + update
        return (new_high, denominator, accumulated)

    start_state = (
        jnp.full((head_count, first_rows), -jnp.inf, jnp.float32),
        jnp.zeros((head_count, first_rows), jnp.float32),
        jnp.zeros((first_rows, head_count, VDIM), jnp.float32),
    )
    quarter = first_rows // tp_count
    offset = lax.axis_index("tp") * quarter
    own_latent = lax.dynamic_slice_in_dim(kv_normed, offset, quarter, 0)
    own_rot = lax.dynamic_slice_in_dim(key_rot, offset, quarter, 0)
    all_latent, all_rot = (
        lax.all_gather(own_latent, ("ep", "tp"), axis=0, tiled=True),
        lax.all_gather(own_rot, ("ep", "tp"), axis=0, tiled=True),
    )
    total_keys = all_latent.shape[0]
    key_block = math.gcd(total_keys, 512)
    latent_blocks = all_latent.reshape(total_keys // key_block, key_block, all_latent.shape[1])
    rot_blocks = all_rot.reshape(total_keys // key_block, key_block, all_rot.shape[1])

    def scan_step(carried, block_pair):
        projected = jnp.dot(
            block_pair[0], keyval_weight, preferred_element_type=jnp.float32
        ).astype(jnp.bfloat16)
        return (attend(carried, (projected, block_pair[1])), None)

    final_state, _ = lax.scan(scan_step, start_state, (latent_blocks, rot_blocks))
    denominator = final_state[1]
    accumulated = final_state[2]
    attended = (
        (accumulated / denominator.T[..., None])
        .astype(jnp.bfloat16)
        .reshape(first_rows, head_count * VDIM)
    )
    mixture = lax.psum_scatter(
        jnp.dot(attended, output_weight, preferred_element_type=jnp.float32).astype(jnp.bfloat16),
        "tp",
        scatter_dimension=0,
        tiled=True,
    ).astype(jnp.float32)
    mixed = rms_scale(mixture, output_gain)
    tok_rows = second_rows.shape[0]
    model_width = second_rows.shape[1]
    top_count = route_ids.shape[1]
    local_count = gate_weight.shape[0]
    expert_count = local_count * ep_count
    capacity = max(tp_count, tok_rows * top_count * 2 // expert_count // tp_count * tp_count)
    normed = rms_scale(second_rows, second_gain)
    flat_ids = route_ids.reshape(-1)
    onehot = (flat_ids[:, None] == jnp.arange(expert_count, dtype=jnp.int32)[None, :]).astype(
        jnp.int32
    )
    slot_rank = jnp.sum((jnp.cumsum(onehot, 0) - 1) * onehot, 1)
    owners = jnp.arange(tok_rows * top_count, dtype=jnp.int32) // top_count
    slot_table = (
        jnp.full((expert_count * capacity,), tok_rows, jnp.int32)
        .at[flat_ids * capacity + slot_rank]
        .set(owners)
    )
    padded = jnp.concatenate([normed, jnp.zeros((1, model_width), jnp.bfloat16)], 0)
    outgoing = padded[slot_table].reshape(ep_count, local_count, capacity, model_width)
    weights = route_weights.reshape(-1, 1)
    shared_hidden = (
        jax.nn.silu(jnp.dot(normed, shared_gate, preferred_element_type=jnp.float32))
        * jnp.dot(normed, shared_up, preferred_element_type=jnp.float32)
    ).astype(jnp.bfloat16)
    shared_part = jnp.dot(shared_hidden, shared_down, preferred_element_type=jnp.float32)
    arrived = lax.all_to_all(outgoing, "ep", split_axis=0, concat_axis=0, tiled=True)
    gate_act = jnp.einsum(
        "sicd,idf->sicf", arrived, gate_weight, preferred_element_type=jnp.float32
    )
    up_act = jnp.einsum("sicd,idf->sicf", arrived, up_weight, preferred_element_type=jnp.float32)
    hidden = (jax.nn.silu(gate_act) * up_act).astype(jnp.bfloat16)
    slot_terms = jnp.einsum(
        "sicf,ifd->sicd", hidden, down_weight, preferred_element_type=jnp.float32
    ).reshape(-1, model_width)
    slot_sum, shared_sum = (
        lax.psum_scatter(
            slot_terms.astype(jnp.bfloat16), "tp", scatter_dimension=1, tiled=True
        ).astype(jnp.float32),
        lax.psum_scatter(
            shared_part.astype(jnp.bfloat16), "tp", scatter_dimension=1, tiled=True
        ).astype(jnp.float32),
    )
    column_part = model_width // tp_count
    returned = lax.all_to_all(
        slot_sum.astype(jnp.bfloat16).reshape(ep_count, local_count * capacity, column_part),
        "ep",
        split_axis=0,
        concat_axis=0,
        tiled=True,
    )
    returned = returned.reshape(expert_count * capacity, column_part)
    picked = returned[flat_ids * capacity + slot_rank].astype(jnp.float32) * weights
    routed = jnp.sum(picked.reshape(tok_rows, top_count, column_part), 1)
    expert_mix = (routed + shared_sum).astype(jnp.bfloat16)
    return (mixed, expert_mix)


def experts_kernel(
    tp_count,
    blocks,
    rows_ref,
    scale_ref,
    gate_ref,
    up_ref,
    down_ref,
    shared_gate_ref,
    shared_up_ref,
    shared_down_ref,
    out_ref,
    total,
):
    step = pl.program_id(0)
    me = lax.axis_index("ep")
    tile = rows_ref.shape[0]
    block_rows = tile // blocks
    width = down_ref.shape[1]
    part = width // tp_count
    rows = rows_ref[...]
    gate_act = jnp.dot(rows, gate_ref[...], preferred_element_type=jnp.float32)
    up_act = jnp.dot(rows, up_ref[...], preferred_element_type=jnp.float32)
    hidden = gate_act / (1.0 + jnp.exp(-gate_act)) * up_act * scale_ref[...]
    total[...] = jnp.dot(
        hidden.astype(jnp.bfloat16), down_ref[...], preferred_element_type=jnp.float32
    )

    for block in range(blocks):

        @pl.when(step * blocks + block == me)
        def _():
            span = pl.ds(block * block_rows, block_rows)
            own = rows_ref[span, :]
            gate_own = jnp.dot(own, shared_gate_ref[...], preferred_element_type=jnp.float32)
            up_own = jnp.dot(own, shared_up_ref[...], preferred_element_type=jnp.float32)
            hidden_own = gate_own / (1.0 + jnp.exp(-gate_own)) * up_own
            total[span, :] += jnp.dot(
                hidden_own.astype(jnp.bfloat16),
                shared_down_ref[...],
                preferred_element_type=jnp.float32,
            )

    for block in range(blocks):
        for column in range(tp_count):
            out_ref[pl.ds((block * tp_count + column) * block_rows, block_rows), :] = total[
                block * block_rows : (block + 1) * block_rows, column * part : (column + 1) * part
            ].astype(jnp.bfloat16)


def run_experts(rows, scale, gate, up, down, shared_gate, shared_up, shared_down, ep_count, tp_count):
    count, width = rows.shape
    block_rows = count // ep_count
    blocks = math.gcd(ep_count, 2)
    tile = block_rows * blocks
    part = width // tp_count

    def whole(array):
        return pl.BlockSpec(array.shape, lambda i: (0, 0))

    return pl.pallas_call(
        functools.partial(experts_kernel, tp_count, blocks),
        out_shape=jax.ShapeDtypeStruct((count * tp_count, part), jnp.bfloat16),
        grid=(count // tile,),
        in_specs=[
            pl.BlockSpec((tile, width), lambda i: (i, 0)),
            pl.BlockSpec((tile, 1), lambda i: (i, 0)),
            whole(gate),
            whole(up),
            whole(down),
            whole(shared_gate),
            whole(shared_up),
            whole(shared_down),
        ],
        out_specs=pl.BlockSpec((tile * tp_count, part), lambda i: (i, 0)),
        scratch_shapes=[pltpu.VMEM((tile, width), jnp.float32)],
        compiler_params=pltpu.CompilerParams(
            dimension_semantics=("arbitrary",), vmem_limit_bytes=48 * 1024 * 1024
        ),
        cost_estimate=pl.CostEstimate(
            flops=6 * count * width * gate.shape[1],
            bytes_accessed=4 * count * width + 6 * width * gate.shape[1],
            transcendentals=count * gate.shape[1],
        ),
    )(rows, scale, gate, up, down, shared_gate, shared_up, shared_down)


def per_device_dense(
    query_latent,
    keyval_latent,
    rotary_key,
    query_gain,
    keyval_gain,
    query_weight,
    keyval_weight,
    output_weight,
    output_gain,
    second_rows,
    second_gain,
    route_ids,
    route_weights,
    gate_weight,
    up_weight,
    down_weight,
    shared_gate,
    shared_up,
    shared_down,
):
    first_rows = query_latent.shape[0]
    tp_count = lax.axis_size("tp")
    ep_count = lax.axis_size("ep")
    head_count = query_weight.shape[1] // (NOPE + ROPE)
    start_row = lax.axis_index("ep") * first_rows
    quarter = first_rows // tp_count
    offset = lax.axis_index("tp") * quarter
    second_quarter = second_rows.shape[0] // tp_count
    second_offset = lax.axis_index("tp") * second_quarter

    own_latent = rms_scale(
        lax.dynamic_slice_in_dim(keyval_latent, offset, quarter, 0), keyval_gain
    )
    own_positions = (start_row + offset).astype(jnp.float32) + jnp.arange(
        quarter, dtype=jnp.float32
    )
    own_rot = rotate(
        lax.dynamic_slice_in_dim(rotary_key, offset, quarter, 0).astype(jnp.float32),
        own_positions,
    ).astype(jnp.bfloat16)
    ids = lax.dynamic_slice_in_dim(route_ids, second_offset, second_quarter, 0)
    wts = lax.dynamic_slice_in_dim(route_weights, second_offset, second_quarter, 0)
    dense = jnp.sum(
        jnp.where(
            ids[:, :, None] == jnp.arange(ep_count, dtype=jnp.int32)[None, None, :],
            wts[:, :, None],
            0.0,
        ),
        1,
    )
    dense_high = dense.astype(jnp.bfloat16)
    dense_low = (dense - dense_high.astype(jnp.float32)).astype(jnp.bfloat16)
    latent_width = own_latent.shape[1]
    used = latent_width + ROPE + 2 * ep_count
    fill = -used % 128
    packed = jnp.concatenate(
        [own_latent, own_rot, dense_high, dense_low, jnp.zeros((quarter, fill), jnp.bfloat16)], 1
    )
    packed = lax.all_gather(packed, ("ep", "tp"), axis=0, tiled=True)
    own_normed = rms_scale(
        lax.dynamic_slice_in_dim(second_rows, second_offset, second_quarter, 0), second_gain
    )
    own_normed, packed = lax.optimization_barrier((own_normed, packed))
    normed = lax.all_gather(own_normed, ("ep", "tp"), axis=0, tiled=True)

    positions = start_row.astype(jnp.float32) + jnp.arange(first_rows, dtype=jnp.float32)
    queries = jnp.dot(
        rms_scale(query_latent, query_gain), query_weight, preferred_element_type=jnp.float32
    ).reshape(first_rows, head_count, NOPE + ROPE)
    queries = jnp.concatenate(
        [queries[..., :NOPE], rotate(queries[..., NOPE:], positions)], -1
    ).astype(jnp.bfloat16)
    all_latent = packed[:, :latent_width]
    all_rot = packed[:, latent_width : latent_width + ROPE]
    total_keys = packed.shape[0]
    keyvals = (
        jnp.dot(all_latent, keyval_weight, preferred_element_type=jnp.float32)
        .astype(jnp.bfloat16)
        .reshape(total_keys, head_count, NOPE + VDIM)
    )
    keys = jnp.concatenate(
        [
            keyvals[..., :NOPE],
            jnp.broadcast_to(all_rot[:, None, :], (total_keys, head_count, ROPE)),
        ],
        -1,
    )
    scores = jnp.einsum("qhd,khd->hqk", queries, keys, preferred_element_type=jnp.float32) * (
        (NOPE + ROPE) ** (-0.5)
    )
    exponent = jnp.exp(scores - jnp.max(scores, -1, keepdims=True))
    denominator = jnp.sum(exponent, -1)
    accumulated = jnp.einsum(
        "hqk,khe->qhe",
        exponent.astype(jnp.bfloat16),
        keyvals[..., NOPE:],
        preferred_element_type=jnp.float32,
    )
    attended = (
        (accumulated / denominator.T[..., None])
        .astype(jnp.bfloat16)
        .reshape(first_rows, head_count * VDIM)
    )
    head_part = jnp.dot(attended, output_weight, preferred_element_type=jnp.float32).astype(
        jnp.bfloat16
    )
    mixture = lax.psum_scatter(head_part, "tp", scatter_dimension=0, tiled=True).astype(
        jnp.float32
    )
    mixed = rms_scale(mixture, output_gain)

    me = lax.axis_index("ep")
    high = lax.dynamic_slice_in_dim(packed, latent_width + ROPE + me, 1, 1)
    low = lax.dynamic_slice_in_dim(packed, latent_width + ROPE + ep_count + me, 1, 1)
    scale = high.astype(jnp.float32) + low.astype(jnp.float32)
    parts = run_experts(
        normed,
        scale,
        gate_weight[0],
        up_weight[0],
        down_weight[0],
        shared_gate,
        shared_up,
        shared_down,
        ep_count,
        tp_count,
    )
    expert_mix = lax.psum_scatter(parts, ("ep", "tp"), scatter_dimension=0, tiled=True)
    return (mixed, expert_mix)


def solution(mesh):
    placed = (
        P("ep", None),
        P("ep", None),
        P("ep", None),
        P(),
        P(),
        P(None, "tp"),
        P(None, "tp"),
        P("tp", None),
        P(),
        P("ep", None),
        P(),
        P("ep", None),
        P("ep", None),
        P("ep", None, "tp"),
        P("ep", None, "tp"),
        P("ep", "tp", None),
        P(None, "tp"),
        P(None, "tp"),
        P("tp", None),
    )
    def per_device(*args):
        tok_rows, top_count = args[11].shape
        expert_count = args[13].shape[0] * mesh.shape["ep"]
        capacity = tok_rows * top_count * 2 // expert_count
        if args[13].shape[0] == 1 and capacity >= tok_rows:
            return per_device_dense(*args)
        return per_device_slots(*args)

    return jax.shard_map(
        per_device,
        mesh=mesh,
        in_specs=placed,
        out_specs=(P(("ep", "tp"), None), P("ep", "tp")),
        check_vma=False,
    )
```

```python
import functools
import math

import jax
import jax.numpy as jnp
from jax import lax
from jax.experimental import pallas as pl
from jax.experimental.pallas import tpu as pltpu
from jax.sharding import PartitionSpec as P

NOPE = 64
ROPE = 32
VDIM = 64


EPS = 1e-06
ROPE_BASE = 10000.0


def rms_scale(values, gain_vec):
    widened = values.astype(jnp.float32)
    normed = widened * lax.rsqrt(jnp.mean(widened * widened, -1, keepdims=True) + EPS)
    return (normed * gain_vec).astype(jnp.bfloat16)


def rotate(values, positions):
    half_width = values.shape[-1] // 2
    inverse = 1.0 / ROPE_BASE ** (
        jnp.arange(half_width, dtype=jnp.float32) * 2.0 / (2 * half_width)
    )
    angles = positions[:, None] * inverse[None, :]
    cosine = jnp.cos(angles)
    sine_vals = jnp.sin(angles)
    if values.ndim == 3:
        cosine = cosine[:, None, :]
        sine_vals = sine_vals[:, None, :]
    first_half = values[..., :half_width]
    second = values[..., half_width:]
    return jnp.concatenate(
        [first_half * cosine - second * sine_vals, first_half * sine_vals + second * cosine], -1
    )


def per_device_slots(
    query_latent,
    keyval_latent,
    rotary_key,
    query_gain,
    keyval_gain,
    query_weight,
    keyval_weight,
    output_weight,
    output_gain,
    second_rows,
    second_gain,
    route_ids,
    route_weights,
    gate_weight,
    up_weight,
    down_weight,
    shared_gate,
    shared_up,
    shared_down,
):
    first_rows = query_latent.shape[0]
    tp_count = lax.axis_size("tp")
    ep_count = lax.axis_size("ep")
    head_count = query_weight.shape[1] // (NOPE + ROPE)
    positions = (lax.axis_index("ep") * first_rows).astype(jnp.float32) + jnp.arange(
        first_rows, dtype=jnp.float32
    )
    queries = jnp.dot(
        rms_scale(query_latent, query_gain), query_weight, preferred_element_type=jnp.float32
    ).reshape(first_rows, head_count, NOPE + ROPE)
    queries = jnp.concatenate(
        [queries[..., :NOPE], rotate(queries[..., NOPE:], positions)], -1
    ).astype(jnp.bfloat16)
    query_plain = queries[..., :NOPE]
    query_turned = queries[..., NOPE:]
    kv_normed = rms_scale(keyval_latent, keyval_gain)
    key_rot = rotate(rotary_key.astype(jnp.float32), positions).astype(jnp.bfloat16)
    score_scale = (NOPE + ROPE) ** (-0.5)

    def attend(carried, pieces):
        highest, denominator, accumulated = carried
        keyval_piece, rot_piece = pieces
        key_count = keyval_piece.shape[0]
        keyval_heads = keyval_piece.reshape(key_count, head_count, NOPE + VDIM)
        scores = jnp.einsum(
            "qhd,khd->hqk",
            query_plain,
            keyval_heads[..., :NOPE],
            preferred_element_type=jnp.float32,
        )
        scores = (
            scores
            + jnp.einsum("qhr,kr->hqk", query_turned, rot_piece, preferred_element_type=jnp.float32)
        ) * score_scale
        new_high = jnp.maximum(highest, jnp.max(scores, -1))
        exponent = jnp.exp(scores - new_high[..., None])
        rescale = jnp.exp(highest - new_high)
        denominator = denominator * rescale + jnp.sum(exponent, -1)
        update = jnp.einsum(
            "hqk,khe->qhe",
            exponent.astype(jnp.bfloat16),
            keyval_heads[..., NOPE:],
            preferred_element_type=jnp.float32,
        )
        accumulated = accumulated * rescale.T[..., None] + update
        return (new_high, denominator, accumulated)

    start_state = (
        jnp.full((head_count, first_rows), -jnp.inf, jnp.float32),
        jnp.zeros((head_count, first_rows), jnp.float32),
        jnp.zeros((first_rows, head_count, VDIM), jnp.float32),
    )
    quarter = first_rows // tp_count
    offset = lax.axis_index("tp") * quarter
    own_latent = lax.dynamic_slice_in_dim(kv_normed, offset, quarter, 0)
    own_rot = lax.dynamic_slice_in_dim(key_rot, offset, quarter, 0)
    all_latent, all_rot = (
        lax.all_gather(own_latent, ("ep", "tp"), axis=0, tiled=True),
        lax.all_gather(own_rot, ("ep", "tp"), axis=0, tiled=True),
    )
    total_keys = all_latent.shape[0]
    key_block = math.gcd(total_keys, 512)
    latent_blocks = all_latent.reshape(total_keys // key_block, key_block, all_latent.shape[1])
    rot_blocks = all_rot.reshape(total_keys // key_block, key_block, all_rot.shape[1])

    def scan_step(carried, block_pair):
        projected = jnp.dot(
            block_pair[0], keyval_weight, preferred_element_type=jnp.float32
        ).astype(jnp.bfloat16)
        return (attend(carried, (projected, block_pair[1])), None)

    final_state, _ = lax.scan(scan_step, start_state, (latent_blocks, rot_blocks))
    denominator = final_state[1]
    accumulated = final_state[2]
    attended = (
        (accumulated / denominator.T[..., None])
        .astype(jnp.bfloat16)
        .reshape(first_rows, head_count * VDIM)
    )
    mixture = lax.psum_scatter(
        jnp.dot(attended, output_weight, preferred_element_type=jnp.float32).astype(jnp.bfloat16),
        "tp",
        scatter_dimension=0,
        tiled=True,
    ).astype(jnp.float32)
    mixed = rms_scale(mixture, output_gain)
    tok_rows = second_rows.shape[0]
    model_width = second_rows.shape[1]
    top_count = route_ids.shape[1]
    local_count = gate_weight.shape[0]
    expert_count = local_count * ep_count
    capacity = max(tp_count, tok_rows * top_count * 2 // expert_count // tp_count * tp_count)
    normed = rms_scale(second_rows, second_gain)
    flat_ids = route_ids.reshape(-1)
    onehot = (flat_ids[:, None] == jnp.arange(expert_count, dtype=jnp.int32)[None, :]).astype(
        jnp.int32
    )
    slot_rank = jnp.sum((jnp.cumsum(onehot, 0) - 1) * onehot, 1)
    owners = jnp.arange(tok_rows * top_count, dtype=jnp.int32) // top_count
    slot_table = (
        jnp.full((expert_count * capacity,), tok_rows, jnp.int32)
        .at[flat_ids * capacity + slot_rank]
        .set(owners)
    )
    padded = jnp.concatenate([normed, jnp.zeros((1, model_width), jnp.bfloat16)], 0)
    outgoing = padded[slot_table].reshape(ep_count, local_count, capacity, model_width)
    weights = route_weights.reshape(-1, 1)
    shared_hidden = (
        jax.nn.silu(jnp.dot(normed, shared_gate, preferred_element_type=jnp.float32))
        * jnp.dot(normed, shared_up, preferred_element_type=jnp.float32)
    ).astype(jnp.bfloat16)
    shared_part = jnp.dot(shared_hidden, shared_down, preferred_element_type=jnp.float32)
    arrived = lax.all_to_all(outgoing, "ep", split_axis=0, concat_axis=0, tiled=True)
    gate_act = jnp.einsum(
        "sicd,idf->sicf", arrived, gate_weight, preferred_element_type=jnp.float32
    )
    up_act = jnp.einsum("sicd,idf->sicf", arrived, up_weight, preferred_element_type=jnp.float32)
    hidden = (jax.nn.silu(gate_act) * up_act).astype(jnp.bfloat16)
    slot_terms = jnp.einsum(
        "sicf,ifd->sicd", hidden, down_weight, preferred_element_type=jnp.float32
    ).reshape(-1, model_width)
    slot_sum, shared_sum = (
        lax.psum_scatter(
            slot_terms.astype(jnp.bfloat16), "tp", scatter_dimension=1, tiled=True
        ).astype(jnp.float32),
        lax.psum_scatter(
            shared_part.astype(jnp.bfloat16), "tp", scatter_dimension=1, tiled=True
        ).astype(jnp.float32),
    )
    column_part = model_width // tp_count
    returned = lax.all_to_all(
        slot_sum.astype(jnp.bfloat16).reshape(ep_count, local_count * capacity, column_part),
        "ep",
        split_axis=0,
        concat_axis=0,
        tiled=True,
    )
    returned = returned.reshape(expert_count * capacity, column_part)
    picked = returned[flat_ids * capacity + slot_rank].astype(jnp.float32) * weights
    routed = jnp.sum(picked.reshape(tok_rows, top_count, column_part), 1)
    expert_mix = (routed + shared_sum).astype(jnp.bfloat16)
    return (mixed, expert_mix)


MESH = pl.DeviceIdType.MESH


def grid_of(ep_count, tp_count):
    y_count = math.gcd(ep_count, 2)
    k_count = math.gcd(tp_count, 2)
    return (ep_count // y_count, y_count, tp_count // k_count, k_count)


def place_of(dims):
    ep_at, tp_at = lax.axis_index("ep"), lax.axis_index("tp")
    return (
        lax.div(ep_at, dims[1]),
        lax.rem(ep_at, dims[1]),
        lax.div(tp_at, dims[3]),
        lax.rem(tp_at, dims[3]),
    )


def moved(dims, place, dz=0, dy=0, dx=0, dk=0):
    return tuple(
        lax.rem(at + step % size, size) if step % size else at
        for at, step, size in zip(place, (dz, dy, dx, dk), dims)
    )


def device_of(dims, place):
    return (place[0] * dims[1] + place[1], place[2] * dims[3] + place[3])


def block_of(dims, place):
    ep_at, tp_at = device_of(dims, place)
    return ep_at * (dims[2] * dims[3]) + tp_at


def peers_of(dims):
    axes = ("dz", "dy", "dx", "dk")
    return [{axis: step} for axis, size in zip(axes, dims) for step in range(1, size)]


def meet(dims, place):
    barrier = pltpu.get_barrier_semaphore()
    peers = peers_of(dims)
    for peer in peers:
        pl.semaphore_signal(
            barrier,
            inc=1,
            device_id=device_of(dims, moved(dims, place, **peer)),
            device_id_type=MESH,
        )
    pl.semaphore_wait(barrier, len(peers))


def far_first(size):
    return sorted(range(1, size), key=lambda step: -min(step, size - step))


def gather_keys(dims):
    z_count, y_count, x_count, k_count = dims
    keys = []
    for dz in range(z_count):
        keys += [("z", dz, 0, 0, 0)]
        keys += [("x", dz, 0, dx, 0) for dx in range(1, x_count)]
        keys += [("y", dz, dy, 0, 0) for dy in range(1, y_count)]
        for dy in range(y_count):
            for dx in range(x_count):
                if dx and dy:
                    keys += [("p", dz, dy, dx, 0), ("q", dz, dy, dx, 0)]
                keys += [("k", dz, dy, dx, dk) for dk in range(1, k_count)]
    return {key: index for index, key in enumerate(keys)}


def gather_kernel(dims, *refs):
    count = (len(refs) - 2) // 2
    owns, alls, (send_sem, recv_sem) = refs[:count], refs[count : 2 * count], refs[2 * count :]
    keys = gather_keys(dims)
    z_count, y_count, x_count, k_count = dims
    me = place_of(dims)
    meet(dims, me)
    sent = []

    def region(which, place, half):
        rows = owns[which].shape[0]
        begin = pl.multiple_of(block_of(dims, place) * rows, rows)
        if half is None:
            return alls[which].at[pl.ds(begin, rows), :]
        return alls[which].at[pl.ds(begin + half * (rows // 2), rows // 2), :]

    def describe(which, key, source, place, half, target):
        return pltpu.make_async_remote_copy(
            src_ref=source,
            dst_ref=region(which, place, half),
            send_sem=send_sem.at[which, keys[key]],
            recv_sem=recv_sem.at[which, keys[key]],
            device_id=device_of(dims, target),
            device_id_type=MESH,
        )

    def send(which, key, origin, half, **step):
        source = region(which, origin, half)
        if origin is me:
            source = owns[which]
        copy = describe(which, key, source, origin, half, moved(dims, me, **step))
        copy.start()
        sent.append(copy)

    def arrive(which, key, origin, half=None):
        source = region(which, origin, half)
        describe(which, key, source, origin, half, me).wait_recv()

    def back(dz=0, dy=0, dx=0, dk=0):
        if not (dz or dy or dx or dk):
            return me
        return moved(dims, me, -dz, -dy, -dx, -dk)

    def to_partner(which, dz, dy, dx):
        for dk in range(1, k_count):
            send(which, ("k", dz, dy, dx, dk), back(dz, dy, dx), None, dk=dk)

    order = [0] + far_first(z_count)[::-1]
    for which in range(count):
        for dz in far_first(z_count):
            send(which, ("z", dz, 0, 0, 0), me, None, dz=dz)
    for which in range(count):
        for dz in order:
            if dz:
                arrive(which, ("z", dz, 0, 0, 0), back(dz))
            for dx in range(1, x_count):
                send(which, ("x", dz, 0, dx, 0), back(dz), None, dx=dx)
            for dy in range(1, y_count):
                send(which, ("y", dz, dy, 0, 0), back(dz), None, dy=dy)
            to_partner(which, dz, 0, 0)
    for which in range(count):
        alls[which][
            pl.ds(
                pl.multiple_of(block_of(dims, me) * owns[which].shape[0], owns[which].shape[0]),
                owns[which].shape[0],
            ),
            :,
        ] = owns[which][...]
    for which in range(count):
        for dz in order:
            for dx in range(1, x_count):
                arrive(which, ("x", dz, 0, dx, 0), back(dz, 0, dx))
                for dy in range(1, y_count):
                    send(which, ("p", dz, dy, dx, 0), back(dz, 0, dx), 0, dy=dy)
                to_partner(which, dz, 0, dx)
            for dy in range(1, y_count):
                arrive(which, ("y", dz, dy, 0, 0), back(dz, dy, 0))
                for dx in range(1, x_count):
                    send(which, ("q", dz, dy, dx, 0), back(dz, dy, 0), 1, dx=dx)
                to_partner(which, dz, dy, 0)
    for which in range(count):
        for dz in order:
            for dy in range(1, y_count):
                for dx in range(1, x_count):
                    arrive(which, ("p", dz, dy, dx, 0), back(dz, dy, dx), 0)
                    arrive(which, ("q", dz, dy, dx, 0), back(dz, dy, dx), 1)
                    to_partner(which, dz, dy, dx)
    for which in range(count):
        for dz in order:
            for dy in range(y_count):
                for dx in range(x_count):
                    for dk in range(1, k_count):
                        arrive(which, ("k", dz, dy, dx, dk), back(dz, dy, dx, dk))
    for copy in sent:
        copy.wait_send()


def gather_all(arrays, ep_count, tp_count):
    dims = grid_of(ep_count, tp_count)
    semaphores = (len(arrays), len(gather_keys(dims)))
    vmem = pl.BlockSpec(memory_space=pltpu.VMEM)
    return pl.pallas_call(
        functools.partial(gather_kernel, dims),
        out_shape=[
            jax.ShapeDtypeStruct((a.shape[0] * ep_count * tp_count, a.shape[1]), a.dtype)
            for a in arrays
        ],
        in_specs=[vmem] * len(arrays),
        out_specs=[vmem] * len(arrays),
        scratch_shapes=[pltpu.SemaphoreType.DMA(semaphores), pltpu.SemaphoreType.DMA(semaphores)],
        compiler_params=pltpu.CompilerParams(
            collective_id=0, has_side_effects=True, vmem_limit_bytes=32 * 1024 * 1024
        ),
    )(*arrays)


def reduce_keys(dims):
    z_count, y_count, x_count, k_count = dims
    keys = []
    for dz in range(z_count):
        for dy in range(y_count):
            for dx in range(x_count):
                keys += [("k", dz, dy, dx, dk) for dk in range(1, k_count)]
                if dx and dy:
                    keys += [("p", dz, dy, dx), ("q", dz, dy, dx)]
                elif dx:
                    keys += [("x", dz, dx)]
                elif dy:
                    keys += [("y", dz, dy)]
                elif dz:
                    keys += [("z", dz)]
    for dx in range(x_count):
        keys += [("mk", dx, dk) for dk in range(1, k_count)]
        if dx:
            keys += [("mx", dx)]
    return {key: index for index, key in enumerate(keys)}


def reduce_slots(dims):
    slots = {}
    for key in reduce_keys(dims):
        group = "pq" if key[0] in "pq" else ("m" if key[0][0] == "m" else "full")
        taken = sum(1 for other in slots.values() if other[0] == group)
        slots[key] = (group, taken)
    sizes = {
        group: max(1, sum(1 for other in slots.values() if other[0] == group))
        for group in ("pq", "m", "full")
    }
    return slots, sizes


def reduce_kernel(
    dims,
    parts_ref,
    head_ref,
    gain_ref,
    mixed_ref,
    out_ref,
    full,
    halves,
    mixes,
    sums,
    mix_sums,
    send_sem,
    recv_sem,
):
    keys = reduce_keys(dims)
    slots, _ = reduce_slots(dims)
    stores = {"pq": halves, "m": mixes, "full": full}
    z_count, y_count, x_count, k_count = dims
    me = place_of(dims)
    rows = out_ref.shape[0]
    half_rows = rows // 2
    mix_rows = mixed_ref.shape[0]
    meet(dims, me)
    sent = []

    def landing(key):
        group, index = slots[key]
        return stores[group].at[index]

    def describe(key, source, target):
        return pltpu.make_async_remote_copy(
            src_ref=source,
            dst_ref=landing(key),
            send_sem=send_sem.at[keys[key]],
            recv_sem=recv_sem.at[keys[key]],
            device_id=device_of(dims, target),
            device_id_type=MESH,
        )

    def send(key, source, **step):
        copy = describe(key, source, moved(dims, me, **step))
        copy.start()
        sent.append(copy)

    def landed(key):
        describe(key, landing(key), me).wait_recv()
        return landing(key)[...].astype(jnp.float32)

    def part_span(dz, dy, dx, dk):
        begin = block_of(dims, moved(dims, me, dz, dy, dx, dk)) * rows
        return pl.ds(pl.multiple_of(begin, rows), rows)

    def mix_span(dx, dk):
        begin = device_of(dims, moved(dims, me, dx=dx, dk=dk))[1] * mix_rows
        return pl.ds(pl.multiple_of(begin, mix_rows), mix_rows)

    z_order = far_first(z_count) + [0]
    z_steps = z_order
    diagonal = [
        (dz, dy, dx) for dz in z_steps for dy in range(1, y_count) for dx in range(1, x_count)
    ]
    side_x = [(dz, 0, dx) for dz in z_steps for dx in range(1, x_count)]
    side_y = [(dz, dy, 0) for dz in z_steps for dy in range(1, y_count)]
    straight = [(dz, 0, 0) for dz in z_steps]

    for place in diagonal[:1]:
        for dk in range(1, k_count):
            send(("k", *place, dk), parts_ref.at[part_span(*place, dk)], dk=dk)
    for dx in range(x_count):
        for dk in range(1, k_count):
            send(("mk", dx, dk), head_ref.at[mix_span(dx, dk)], dk=dk)
    for place in diagonal[1:] + side_x + side_y + straight:
        for dk in range(1, k_count):
            send(("k", *place, dk), parts_ref.at[part_span(*place, dk)], dk=dk)

    def core_sum(place):
        value = parts_ref[part_span(*place, 0), :].astype(jnp.float32)
        for dk in range(1, k_count):
            value = value + landed(("k", *place, dk))
        return value

    index_of = {}

    def keep(place, value):
        index_of[place] = len(index_of)
        sums[index_of[place]] = value.astype(jnp.bfloat16)
        return index_of[place]

    def mix_core(dx):
        value = head_ref[mix_span(dx, 0), :].astype(jnp.float32)
        for dk in range(1, k_count):
            value = value + landed(("mk", dx, dk))
        return value

    for dx in range(1, x_count):
        mix_sums[dx - 1] = mix_core(dx).astype(jnp.bfloat16)
        send(("mx", dx), mix_sums.at[dx - 1], dx=dx)
    for place in diagonal:
        dz, dy, dx = place
        index = keep(place, core_sum(place))
        send(("p", dz, dy, dx), sums.at[index, pl.ds(0, half_rows)], dy=dy)
        send(("q", dz, dy, dx), sums.at[index, pl.ds(half_rows, half_rows)], dx=dx)
    for dz in z_steps:
        for dx in range(1, x_count):
            value = core_sum((dz, 0, dx))
            upper, lower = value[:half_rows], value[half_rows:]
            for dy in range(1, y_count):
                upper = upper + landed(("p", dz, dy, dx))
            index = keep((dz, 0, dx), jnp.concatenate([upper, lower], 0))
            send(("x", dz, dx), sums.at[index], dx=dx)
        for dy in range(1, y_count):
            value = core_sum((dz, dy, 0))
            upper, lower = value[:half_rows], value[half_rows:]
            for dx in range(1, x_count):
                lower = lower + landed(("q", dz, dy, dx))
            index = keep((dz, dy, 0), jnp.concatenate([upper, lower], 0))
            send(("y", dz, dy), sums.at[index], dy=dy)
    mixture = mix_core(0)
    for dx in range(1, x_count):
        mixture = mixture + landed(("mx", dx))
    scale = lax.rsqrt(jnp.mean(mixture * mixture, -1, keepdims=True) + EPS)
    mixed_ref[...] = (mixture * scale * gain_ref[...]).astype(jnp.bfloat16)
    for dz in z_steps:
        value = core_sum((dz, 0, 0))
        for dx in range(1, x_count):
            value = value + landed(("x", dz, dx))
        for dy in range(1, y_count):
            value = value + landed(("y", dz, dy))
        if dz:
            index = keep((dz, 0, 0), value)
            send(("z", dz), sums.at[index], dz=dz)
    for dz in range(1, z_count):
        value = value + landed(("z", dz))
    out_ref[...] = value.astype(jnp.bfloat16)
    for copy in sent:
        copy.wait_send()


def reduce_all(parts, head_part, gain, ep_count, tp_count):
    dims = grid_of(ep_count, tp_count)
    _, sizes = reduce_slots(dims)
    rows = parts.shape[0] // (ep_count * tp_count)
    width = parts.shape[1]
    mix_rows = head_part.shape[0] // tp_count
    mix_width = head_part.shape[1]
    vmem = pl.BlockSpec(memory_space=pltpu.VMEM)
    semaphores = pltpu.SemaphoreType.DMA((len(reduce_keys(dims)),))
    return pl.pallas_call(
        functools.partial(reduce_kernel, dims),
        out_shape=[
            jax.ShapeDtypeStruct((mix_rows, mix_width), jnp.bfloat16),
            jax.ShapeDtypeStruct((rows, width), jnp.bfloat16),
        ],
        in_specs=[vmem] * 3,
        out_specs=[vmem] * 2,
        scratch_shapes=[
            pltpu.VMEM((sizes["full"], rows, width), jnp.bfloat16),
            pltpu.VMEM((sizes["pq"], rows // 2, width), jnp.bfloat16),
            pltpu.VMEM((sizes["m"], mix_rows, mix_width), jnp.bfloat16),
            pltpu.VMEM((dims[0] * dims[1] * dims[2], rows, width), jnp.bfloat16),
            pltpu.VMEM((max(1, dims[2] - 1), mix_rows, mix_width), jnp.bfloat16),
            semaphores,
            semaphores,
        ],
        compiler_params=pltpu.CompilerParams(
            collective_id=1, has_side_effects=True, vmem_limit_bytes=48 * 1024 * 1024
        ),
    )(parts, head_part, gain)


def experts_kernel(
    tp_count,
    blocks,
    rows_ref,
    scale_ref,
    gate_ref,
    up_ref,
    down_ref,
    shared_gate_ref,
    shared_up_ref,
    shared_down_ref,
    out_ref,
    total,
):
    step = pl.program_id(0)
    me = lax.axis_index("ep")
    tile = rows_ref.shape[0]
    block_rows = tile // blocks
    width = down_ref.shape[1]
    part = width // tp_count
    rows = rows_ref[...]
    gate_act = jnp.dot(rows, gate_ref[...], preferred_element_type=jnp.float32)
    up_act = jnp.dot(rows, up_ref[...], preferred_element_type=jnp.float32)
    hidden = gate_act / (1.0 + jnp.exp(-gate_act)) * up_act * scale_ref[...]
    total[...] = jnp.dot(
        hidden.astype(jnp.bfloat16), down_ref[...], preferred_element_type=jnp.float32
    )

    for block in range(blocks):

        @pl.when(step * blocks + block == me)
        def _():
            span = pl.ds(block * block_rows, block_rows)
            own = rows_ref[span, :]
            gate_own = jnp.dot(own, shared_gate_ref[...], preferred_element_type=jnp.float32)
            up_own = jnp.dot(own, shared_up_ref[...], preferred_element_type=jnp.float32)
            hidden_own = gate_own / (1.0 + jnp.exp(-gate_own)) * up_own
            total[span, :] += jnp.dot(
                hidden_own.astype(jnp.bfloat16),
                shared_down_ref[...],
                preferred_element_type=jnp.float32,
            )

    for block in range(blocks):
        for column in range(tp_count):
            out_ref[pl.ds((block * tp_count + column) * block_rows, block_rows), :] = total[
                block * block_rows : (block + 1) * block_rows, column * part : (column + 1) * part
            ].astype(jnp.bfloat16)


def run_experts(rows, scale, gate, up, down, shared_gate, shared_up, shared_down, ep_count, tp_count):
    count, width = rows.shape
    block_rows = count // ep_count
    blocks = math.gcd(ep_count, 2)
    tile = block_rows * blocks
    part = width // tp_count

    def whole(array):
        return pl.BlockSpec(array.shape, lambda i: (0, 0))

    return pl.pallas_call(
        functools.partial(experts_kernel, tp_count, blocks),
        out_shape=jax.ShapeDtypeStruct((count * tp_count, part), jnp.bfloat16),
        grid=(count // tile,),
        in_specs=[
            pl.BlockSpec((tile, width), lambda i: (i, 0)),
            pl.BlockSpec((tile, 1), lambda i: (i, 0)),
            whole(gate),
            whole(up),
            whole(down),
            whole(shared_gate),
            whole(shared_up),
            whole(shared_down),
        ],
        out_specs=pl.BlockSpec((tile * tp_count, part), lambda i: (i, 0)),
        scratch_shapes=[pltpu.VMEM((tile, width), jnp.float32)],
        compiler_params=pltpu.CompilerParams(
            dimension_semantics=("arbitrary",), vmem_limit_bytes=48 * 1024 * 1024
        ),
        cost_estimate=pl.CostEstimate(
            flops=6 * count * width * gate.shape[1],
            bytes_accessed=4 * count * width + 6 * width * gate.shape[1],
            transcendentals=count * gate.shape[1],
        ),
    )(rows, scale, gate, up, down, shared_gate, shared_up, shared_down)


def per_device_dense(
    query_latent,
    keyval_latent,
    rotary_key,
    query_gain,
    keyval_gain,
    query_weight,
    keyval_weight,
    output_weight,
    output_gain,
    second_rows,
    second_gain,
    route_ids,
    route_weights,
    gate_weight,
    up_weight,
    down_weight,
    shared_gate,
    shared_up,
    shared_down,
):
    first_rows = query_latent.shape[0]
    tp_count = lax.axis_size("tp")
    ep_count = lax.axis_size("ep")
    head_count = query_weight.shape[1] // (NOPE + ROPE)
    start_row = lax.axis_index("ep") * first_rows
    quarter = first_rows // tp_count
    offset = lax.axis_index("tp") * quarter
    second_quarter = second_rows.shape[0] // tp_count
    second_offset = lax.axis_index("tp") * second_quarter

    own_latent = rms_scale(
        lax.dynamic_slice_in_dim(keyval_latent, offset, quarter, 0), keyval_gain
    )
    own_positions = (start_row + offset).astype(jnp.float32) + jnp.arange(
        quarter, dtype=jnp.float32
    )
    own_rot = rotate(
        lax.dynamic_slice_in_dim(rotary_key, offset, quarter, 0).astype(jnp.float32),
        own_positions,
    ).astype(jnp.bfloat16)
    ids = lax.dynamic_slice_in_dim(route_ids, second_offset, second_quarter, 0)
    wts = lax.dynamic_slice_in_dim(route_weights, second_offset, second_quarter, 0)
    dense = jnp.sum(
        jnp.where(
            ids[:, :, None] == jnp.arange(ep_count, dtype=jnp.int32)[None, None, :],
            wts[:, :, None],
            0.0,
        ),
        1,
    )
    dense_high = dense.astype(jnp.bfloat16)
    dense_low = (dense - dense_high.astype(jnp.float32)).astype(jnp.bfloat16)
    latent_width = own_latent.shape[1]
    used = latent_width + ROPE + 2 * ep_count
    fill = -used % 128
    packed = jnp.concatenate(
        [own_latent, own_rot, dense_high, dense_low, jnp.zeros((quarter, fill), jnp.bfloat16)], 1
    )
    own_normed = rms_scale(
        lax.dynamic_slice_in_dim(second_rows, second_offset, second_quarter, 0), second_gain
    )
    packed, normed = gather_all([packed, own_normed], ep_count, tp_count)

    positions = start_row.astype(jnp.float32) + jnp.arange(first_rows, dtype=jnp.float32)
    queries = jnp.dot(
        rms_scale(query_latent, query_gain), query_weight, preferred_element_type=jnp.float32
    ).reshape(first_rows, head_count, NOPE + ROPE)
    queries = jnp.concatenate(
        [queries[..., :NOPE], rotate(queries[..., NOPE:], positions)], -1
    ).astype(jnp.bfloat16)
    all_latent = packed[:, :latent_width]
    all_rot = packed[:, latent_width : latent_width + ROPE]
    total_keys = packed.shape[0]
    keyvals = (
        jnp.dot(all_latent, keyval_weight, preferred_element_type=jnp.float32)
        .astype(jnp.bfloat16)
        .reshape(total_keys, head_count, NOPE + VDIM)
    )
    keys = jnp.concatenate(
        [
            keyvals[..., :NOPE],
            jnp.broadcast_to(all_rot[:, None, :], (total_keys, head_count, ROPE)),
        ],
        -1,
    )
    scores = jnp.einsum("qhd,khd->hqk", queries, keys, preferred_element_type=jnp.float32) * (
        (NOPE + ROPE) ** (-0.5)
    )
    exponent = jnp.exp(scores - jnp.max(scores, -1, keepdims=True))
    denominator = jnp.sum(exponent, -1)
    accumulated = jnp.einsum(
        "hqk,khe->qhe",
        exponent.astype(jnp.bfloat16),
        keyvals[..., NOPE:],
        preferred_element_type=jnp.float32,
    )
    attended = (
        (accumulated / denominator.T[..., None])
        .astype(jnp.bfloat16)
        .reshape(first_rows, head_count * VDIM)
    )
    head_part = jnp.dot(attended, output_weight, preferred_element_type=jnp.float32).astype(
        jnp.bfloat16
    )

    me = lax.axis_index("ep")
    high = lax.dynamic_slice_in_dim(packed, latent_width + ROPE + me, 1, 1)
    low = lax.dynamic_slice_in_dim(packed, latent_width + ROPE + ep_count + me, 1, 1)
    scale = high.astype(jnp.float32) + low.astype(jnp.float32)
    parts = run_experts(
        normed,
        scale,
        gate_weight[0],
        up_weight[0],
        down_weight[0],
        shared_gate,
        shared_up,
        shared_down,
        ep_count,
        tp_count,
    )
    mixed, expert_mix = reduce_all(
        parts, head_part, output_gain.reshape(1, -1), ep_count, tp_count
    )
    return (mixed, expert_mix)


def solution(mesh):
    placed = (
        P("ep", None),
        P("ep", None),
        P("ep", None),
        P(),
        P(),
        P(None, "tp"),
        P(None, "tp"),
        P("tp", None),
        P(),
        P("ep", None),
        P(),
        P("ep", None),
        P("ep", None),
        P("ep", None, "tp"),
        P("ep", None, "tp"),
        P("ep", "tp", None),
        P(None, "tp"),
        P(None, "tp"),
        P("tp", None),
    )
    def per_device(*args):
        tok_rows, top_count = args[11].shape
        expert_count = args[13].shape[0] * mesh.shape["ep"]
        capacity = tok_rows * top_count * 2 // expert_count
        if args[13].shape[0] == 1 and capacity >= tok_rows:
            return per_device_dense(*args)
        return per_device_slots(*args)

    return jax.shard_map(
        per_device,
        mesh=mesh,
        in_specs=placed,
        out_specs=(P(("ep", "tp"), None), P("ep", "tp")),
        check_vma=False,
    )
```

```python
import functools
import math

import jax
import jax.numpy as jnp
from jax import lax
from jax.experimental import pallas as pl
from jax.experimental.pallas import tpu as pltpu
from jax.sharding import PartitionSpec as P

NOPE = 64
ROPE = 32
VDIM = 64


EPS = 1e-06
ROPE_BASE = 10000.0


def rms_scale(values, gain_vec):
    widened = values.astype(jnp.float32)
    normed = widened * lax.rsqrt(jnp.mean(widened * widened, -1, keepdims=True) + EPS)
    return (normed * gain_vec).astype(jnp.bfloat16)


def rotate(values, positions):
    half_width = values.shape[-1] // 2
    inverse = 1.0 / ROPE_BASE ** (
        jnp.arange(half_width, dtype=jnp.float32) * 2.0 / (2 * half_width)
    )
    angles = positions[:, None] * inverse[None, :]
    cosine = jnp.cos(angles)
    sine_vals = jnp.sin(angles)
    if values.ndim == 3:
        cosine = cosine[:, None, :]
        sine_vals = sine_vals[:, None, :]
    first_half = values[..., :half_width]
    second = values[..., half_width:]
    return jnp.concatenate(
        [first_half * cosine - second * sine_vals, first_half * sine_vals + second * cosine], -1
    )


def per_device_slots(
    query_latent,
    keyval_latent,
    rotary_key,
    query_gain,
    keyval_gain,
    query_weight,
    keyval_weight,
    output_weight,
    output_gain,
    second_rows,
    second_gain,
    route_ids,
    route_weights,
    gate_weight,
    up_weight,
    down_weight,
    shared_gate,
    shared_up,
    shared_down,
):
    first_rows = query_latent.shape[0]
    tp_count = lax.axis_size("tp")
    ep_count = lax.axis_size("ep")
    head_count = query_weight.shape[1] // (NOPE + ROPE)
    positions = (lax.axis_index("ep") * first_rows).astype(jnp.float32) + jnp.arange(
        first_rows, dtype=jnp.float32
    )
    queries = jnp.dot(
        rms_scale(query_latent, query_gain), query_weight, preferred_element_type=jnp.float32
    ).reshape(first_rows, head_count, NOPE + ROPE)
    queries = jnp.concatenate(
        [queries[..., :NOPE], rotate(queries[..., NOPE:], positions)], -1
    ).astype(jnp.bfloat16)
    query_plain = queries[..., :NOPE]
    query_turned = queries[..., NOPE:]
    kv_normed = rms_scale(keyval_latent, keyval_gain)
    key_rot = rotate(rotary_key.astype(jnp.float32), positions).astype(jnp.bfloat16)
    score_scale = (NOPE + ROPE) ** (-0.5)

    def attend(carried, pieces):
        highest, denominator, accumulated = carried
        keyval_piece, rot_piece = pieces
        key_count = keyval_piece.shape[0]
        keyval_heads = keyval_piece.reshape(key_count, head_count, NOPE + VDIM)
        scores = jnp.einsum(
            "qhd,khd->hqk",
            query_plain,
            keyval_heads[..., :NOPE],
            preferred_element_type=jnp.float32,
        )
        scores = (
            scores
            + jnp.einsum("qhr,kr->hqk", query_turned, rot_piece, preferred_element_type=jnp.float32)
        ) * score_scale
        new_high = jnp.maximum(highest, jnp.max(scores, -1))
        exponent = jnp.exp(scores - new_high[..., None])
        rescale = jnp.exp(highest - new_high)
        denominator = denominator * rescale + jnp.sum(exponent, -1)
        update = jnp.einsum(
            "hqk,khe->qhe",
            exponent.astype(jnp.bfloat16),
            keyval_heads[..., NOPE:],
            preferred_element_type=jnp.float32,
        )
        accumulated = accumulated * rescale.T[..., None] + update
        return (new_high, denominator, accumulated)

    start_state = (
        jnp.full((head_count, first_rows), -jnp.inf, jnp.float32),
        jnp.zeros((head_count, first_rows), jnp.float32),
        jnp.zeros((first_rows, head_count, VDIM), jnp.float32),
    )
    quarter = first_rows // tp_count
    offset = lax.axis_index("tp") * quarter
    own_latent = lax.dynamic_slice_in_dim(kv_normed, offset, quarter, 0)
    own_rot = lax.dynamic_slice_in_dim(key_rot, offset, quarter, 0)
    all_latent, all_rot = (
        lax.all_gather(own_latent, ("ep", "tp"), axis=0, tiled=True),
        lax.all_gather(own_rot, ("ep", "tp"), axis=0, tiled=True),
    )
    total_keys = all_latent.shape[0]
    key_block = math.gcd(total_keys, 512)
    latent_blocks = all_latent.reshape(total_keys // key_block, key_block, all_latent.shape[1])
    rot_blocks = all_rot.reshape(total_keys // key_block, key_block, all_rot.shape[1])

    def scan_step(carried, block_pair):
        projected = jnp.dot(
            block_pair[0], keyval_weight, preferred_element_type=jnp.float32
        ).astype(jnp.bfloat16)
        return (attend(carried, (projected, block_pair[1])), None)

    final_state, _ = lax.scan(scan_step, start_state, (latent_blocks, rot_blocks))
    denominator = final_state[1]
    accumulated = final_state[2]
    attended = (
        (accumulated / denominator.T[..., None])
        .astype(jnp.bfloat16)
        .reshape(first_rows, head_count * VDIM)
    )
    mixture = lax.psum_scatter(
        jnp.dot(attended, output_weight, preferred_element_type=jnp.float32).astype(jnp.bfloat16),
        "tp",
        scatter_dimension=0,
        tiled=True,
    ).astype(jnp.float32)
    mixed = rms_scale(mixture, output_gain)
    tok_rows = second_rows.shape[0]
    model_width = second_rows.shape[1]
    top_count = route_ids.shape[1]
    local_count = gate_weight.shape[0]
    expert_count = local_count * ep_count
    capacity = max(tp_count, tok_rows * top_count * 2 // expert_count // tp_count * tp_count)
    normed = rms_scale(second_rows, second_gain)
    flat_ids = route_ids.reshape(-1)
    onehot = (flat_ids[:, None] == jnp.arange(expert_count, dtype=jnp.int32)[None, :]).astype(
        jnp.int32
    )
    slot_rank = jnp.sum((jnp.cumsum(onehot, 0) - 1) * onehot, 1)
    owners = jnp.arange(tok_rows * top_count, dtype=jnp.int32) // top_count
    slot_table = (
        jnp.full((expert_count * capacity,), tok_rows, jnp.int32)
        .at[flat_ids * capacity + slot_rank]
        .set(owners)
    )
    padded = jnp.concatenate([normed, jnp.zeros((1, model_width), jnp.bfloat16)], 0)
    outgoing = padded[slot_table].reshape(ep_count, local_count, capacity, model_width)
    weights = route_weights.reshape(-1, 1)
    shared_hidden = (
        jax.nn.silu(jnp.dot(normed, shared_gate, preferred_element_type=jnp.float32))
        * jnp.dot(normed, shared_up, preferred_element_type=jnp.float32)
    ).astype(jnp.bfloat16)
    shared_part = jnp.dot(shared_hidden, shared_down, preferred_element_type=jnp.float32)
    arrived = lax.all_to_all(outgoing, "ep", split_axis=0, concat_axis=0, tiled=True)
    gate_act = jnp.einsum(
        "sicd,idf->sicf", arrived, gate_weight, preferred_element_type=jnp.float32
    )
    up_act = jnp.einsum("sicd,idf->sicf", arrived, up_weight, preferred_element_type=jnp.float32)
    hidden = (jax.nn.silu(gate_act) * up_act).astype(jnp.bfloat16)
    slot_terms = jnp.einsum(
        "sicf,ifd->sicd", hidden, down_weight, preferred_element_type=jnp.float32
    ).reshape(-1, model_width)
    slot_sum, shared_sum = (
        lax.psum_scatter(
            slot_terms.astype(jnp.bfloat16), "tp", scatter_dimension=1, tiled=True
        ).astype(jnp.float32),
        lax.psum_scatter(
            shared_part.astype(jnp.bfloat16), "tp", scatter_dimension=1, tiled=True
        ).astype(jnp.float32),
    )
    column_part = model_width // tp_count
    returned = lax.all_to_all(
        slot_sum.astype(jnp.bfloat16).reshape(ep_count, local_count * capacity, column_part),
        "ep",
        split_axis=0,
        concat_axis=0,
        tiled=True,
    )
    returned = returned.reshape(expert_count * capacity, column_part)
    picked = returned[flat_ids * capacity + slot_rank].astype(jnp.float32) * weights
    routed = jnp.sum(picked.reshape(tok_rows, top_count, column_part), 1)
    expert_mix = (routed + shared_sum).astype(jnp.bfloat16)
    return (mixed, expert_mix)


MESH = pl.DeviceIdType.MESH


def grid_of(ep_count, tp_count):
    y_count = math.gcd(ep_count, 2)
    k_count = math.gcd(tp_count, 2)
    return (ep_count // y_count, y_count, tp_count // k_count, k_count)


def place_of(dims):
    ep_at, tp_at = lax.axis_index("ep"), lax.axis_index("tp")
    return (
        lax.div(ep_at, dims[1]),
        lax.rem(ep_at, dims[1]),
        lax.div(tp_at, dims[3]),
        lax.rem(tp_at, dims[3]),
    )


def moved(dims, place, dz=0, dy=0, dx=0, dk=0):
    return tuple(
        lax.rem(at + step % size, size) if step % size else at
        for at, step, size in zip(place, (dz, dy, dx, dk), dims)
    )


def device_of(dims, place):
    return (place[0] * dims[1] + place[1], place[2] * dims[3] + place[3])


def block_of(dims, place):
    ep_at, tp_at = device_of(dims, place)
    return ep_at * (dims[2] * dims[3]) + tp_at


def peers_of(dims):
    axes = ("dz", "dy", "dx", "dk")
    return [{axis: step} for axis, size in zip(axes, dims) for step in range(1, size)]


def meet(dims, place):
    barrier = pltpu.get_barrier_semaphore()
    peers = peers_of(dims)
    for peer in peers:
        pl.semaphore_signal(
            barrier,
            inc=1,
            device_id=device_of(dims, moved(dims, place, **peer)),
            device_id_type=MESH,
        )
    pl.semaphore_wait(barrier, len(peers))


def far_first(size):
    return sorted(range(1, size), key=lambda step: -min(step, size - step))


def gather_keys(dims):
    z_count, y_count, x_count, k_count = dims
    keys = []
    for dz in range(z_count):
        keys += [("z", dz, 0, 0, 0)]
        keys += [("x", dz, 0, dx, 0) for dx in range(1, x_count)]
        keys += [("y", dz, dy, 0, 0) for dy in range(1, y_count)]
        for dy in range(y_count):
            for dx in range(x_count):
                if dx and dy:
                    keys += [("p", dz, dy, dx, 0), ("q", dz, dy, dx, 0)]
                keys += [("k", dz, dy, dx, dk) for dk in range(1, k_count)]
    return {key: index for index, key in enumerate(keys)}


def gather_kernel(dims, *refs):
    count = (len(refs) - 2) // 2
    owns, alls, (send_sem, recv_sem) = refs[:count], refs[count : 2 * count], refs[2 * count :]
    keys = gather_keys(dims)
    z_count, y_count, x_count, k_count = dims
    me = place_of(dims)
    meet(dims, me)
    sent = []

    def region(which, place, half):
        rows = owns[which].shape[0]
        begin = pl.multiple_of(block_of(dims, place) * rows, rows)
        if half is None:
            return alls[which].at[pl.ds(begin, rows), :]
        return alls[which].at[pl.ds(begin + half * (rows // 2), rows // 2), :]

    def describe(which, key, source, place, half, target):
        return pltpu.make_async_remote_copy(
            src_ref=source,
            dst_ref=region(which, place, half),
            send_sem=send_sem.at[which, keys[key]],
            recv_sem=recv_sem.at[which, keys[key]],
            device_id=device_of(dims, target),
            device_id_type=MESH,
        )

    def send(which, key, origin, half, **step):
        source = region(which, origin, half)
        if origin is me:
            source = owns[which]
        copy = describe(which, key, source, origin, half, moved(dims, me, **step))
        copy.start()
        sent.append(copy)

    def arrive(which, key, origin, half=None):
        source = region(which, origin, half)
        describe(which, key, source, origin, half, me).wait_recv()

    def back(dz=0, dy=0, dx=0, dk=0):
        if not (dz or dy or dx or dk):
            return me
        return moved(dims, me, -dz, -dy, -dx, -dk)

    def to_partner(which, dz, dy, dx):
        for dk in range(1, k_count):
            send(which, ("k", dz, dy, dx, dk), back(dz, dy, dx), None, dk=dk)

    order = [0] + far_first(z_count)[::-1]
    for which in range(count):
        for dz in far_first(z_count):
            send(which, ("z", dz, 0, 0, 0), me, None, dz=dz)
    for which in range(count):
        for dz in order:
            if dz:
                arrive(which, ("z", dz, 0, 0, 0), back(dz))
            for dx in range(1, x_count):
                send(which, ("x", dz, 0, dx, 0), back(dz), None, dx=dx)
            for dy in range(1, y_count):
                send(which, ("y", dz, dy, 0, 0), back(dz), None, dy=dy)
            to_partner(which, dz, 0, 0)
    for which in range(count):
        alls[which][
            pl.ds(
                pl.multiple_of(block_of(dims, me) * owns[which].shape[0], owns[which].shape[0]),
                owns[which].shape[0],
            ),
            :,
        ] = owns[which][...]
    for which in range(count):
        for dz in order:
            for dx in range(1, x_count):
                arrive(which, ("x", dz, 0, dx, 0), back(dz, 0, dx))
                for dy in range(1, y_count):
                    send(which, ("p", dz, dy, dx, 0), back(dz, 0, dx), 0, dy=dy)
                to_partner(which, dz, 0, dx)
            for dy in range(1, y_count):
                arrive(which, ("y", dz, dy, 0, 0), back(dz, dy, 0))
                for dx in range(1, x_count):
                    send(which, ("q", dz, dy, dx, 0), back(dz, dy, 0), 1, dx=dx)
                to_partner(which, dz, dy, 0)
    for which in range(count):
        for dz in order:
            for dy in range(1, y_count):
                for dx in range(1, x_count):
                    arrive(which, ("p", dz, dy, dx, 0), back(dz, dy, dx), 0)
                    arrive(which, ("q", dz, dy, dx, 0), back(dz, dy, dx), 1)
                    to_partner(which, dz, dy, dx)
    for which in range(count):
        for dz in order:
            for dy in range(y_count):
                for dx in range(x_count):
                    for dk in range(1, k_count):
                        arrive(which, ("k", dz, dy, dx, dk), back(dz, dy, dx, dk))
    for copy in sent:
        copy.wait_send()


def gather_all(arrays, ep_count, tp_count):
    dims = grid_of(ep_count, tp_count)
    semaphores = (len(arrays), len(gather_keys(dims)))
    vmem = pl.BlockSpec(memory_space=pltpu.VMEM)
    return pl.pallas_call(
        functools.partial(gather_kernel, dims),
        out_shape=[
            jax.ShapeDtypeStruct((a.shape[0] * ep_count * tp_count, a.shape[1]), a.dtype)
            for a in arrays
        ],
        in_specs=[vmem] * len(arrays),
        out_specs=[vmem] * len(arrays),
        scratch_shapes=[pltpu.SemaphoreType.DMA(semaphores), pltpu.SemaphoreType.DMA(semaphores)],
        compiler_params=pltpu.CompilerParams(
            collective_id=0, has_side_effects=True, vmem_limit_bytes=32 * 1024 * 1024
        ),
    )(*arrays)


def reduce_keys(dims):
    z_count, y_count, x_count, k_count = dims
    keys = []
    for dz in range(z_count):
        for dy in range(y_count):
            for dx in range(x_count):
                keys += [("k", dz, dy, dx, dk) for dk in range(1, k_count)]
                if dx and dy:
                    keys += [("p", dz, dy, dx), ("q", dz, dy, dx)]
                elif dx:
                    keys += [("x", dz, dx)]
                elif dy:
                    keys += [("y", dz, dy)]
                elif dz:
                    keys += [("z", dz)]
    for dx in range(x_count):
        keys += [("mk", dx, dk) for dk in range(1, k_count)]
        if dx:
            keys += [("mx", dx)]
    return {key: index for index, key in enumerate(keys)}


def reduce_slots(dims):
    slots = {}
    for key in reduce_keys(dims):
        group = "pq" if key[0] in "pq" else ("m" if key[0][0] == "m" else "full")
        taken = sum(1 for other in slots.values() if other[0] == group)
        slots[key] = (group, taken)
    sizes = {
        group: max(1, sum(1 for other in slots.values() if other[0] == group))
        for group in ("pq", "m", "full")
    }
    return slots, sizes


def reduce_kernel(
    dims,
    rows_ref,
    scale_ref,
    gate_ref,
    up_ref,
    down_ref,
    shared_gate_ref,
    shared_up_ref,
    shared_down_ref,
    head_ref,
    gain_ref,
    mixed_ref,
    out_ref,
    parts_ref,
    full,
    halves,
    mixes,
    sums,
    mix_sums,
    send_sem,
    recv_sem,
):
    keys = reduce_keys(dims)
    slots, _ = reduce_slots(dims)
    stores = {"pq": halves, "m": mixes, "full": full}
    z_count, y_count, x_count, k_count = dims
    me = place_of(dims)
    rows = out_ref.shape[0]
    half_rows = rows // 2
    mix_rows = mixed_ref.shape[0]
    meet(dims, me)
    sent = []

    def landing(key):
        group, index = slots[key]
        return stores[group].at[index]

    def describe(key, source, target):
        return pltpu.make_async_remote_copy(
            src_ref=source,
            dst_ref=landing(key),
            send_sem=send_sem.at[keys[key]],
            recv_sem=recv_sem.at[keys[key]],
            device_id=device_of(dims, target),
            device_id_type=MESH,
        )

    def send(key, source, **step):
        copy = describe(key, source, moved(dims, me, **step))
        copy.start()
        sent.append(copy)

    def landed(key):
        describe(key, landing(key), me).wait_recv()
        return landing(key)[...].astype(jnp.float32)

    def part_of(dz, dy, dx, dk):
        column = device_of(dims, moved(dims, me, dx=dx, dk=dk))[1]
        return parts_ref.at[dz * y_count + dy, column]

    def compute(dz, dy):
        begin = device_of(dims, moved(dims, me, dz=dz, dy=dy))[0] * rows
        span = pl.ds(pl.multiple_of(begin, rows), rows)
        tokens = rows_ref[span, :]
        gate_act = jnp.dot(tokens, gate_ref[...], preferred_element_type=jnp.float32)
        up_act = jnp.dot(tokens, up_ref[...], preferred_element_type=jnp.float32)
        hidden = gate_act / (1.0 + jnp.exp(-gate_act)) * up_act * scale_ref[span, :]
        hidden = hidden.astype(jnp.bfloat16)
        own = dz == 0 and dy == 0
        if own:
            gate_own = jnp.dot(tokens, shared_gate_ref[...], preferred_element_type=jnp.float32)
            up_own = jnp.dot(tokens, shared_up_ref[...], preferred_element_type=jnp.float32)
            hidden_own = gate_own / (1.0 + jnp.exp(-gate_own)) * up_own
            hidden_own = hidden_own.astype(jnp.bfloat16)
        part = out_ref.shape[1]
        for column in range(x_count * k_count):
            columns = pl.ds(column * part, part)
            value = jnp.dot(hidden, down_ref[:, columns], preferred_element_type=jnp.float32)
            if own:
                value += jnp.dot(
                    hidden_own, shared_down_ref[:, columns], preferred_element_type=jnp.float32
                )
            parts_ref[dz * y_count + dy, column] = value.astype(jnp.bfloat16)
        for dx in range(x_count - 1, -1, -1):
            for dk in range(1, k_count):
                send(("k", dz, dy, dx, dk), part_of(dz, dy, dx, dk), dk=dk)

    def mix_span(dx, dk):
        begin = device_of(dims, moved(dims, me, dx=dx, dk=dk))[1] * mix_rows
        return pl.ds(pl.multiple_of(begin, mix_rows), mix_rows)

    z_steps = far_first(z_count) + [0]
    for dx in range(x_count):
        for dk in range(1, k_count):
            send(("mk", dx, dk), head_ref.at[mix_span(dx, dk)], dk=dk)

    def core_sum(place):
        value = part_of(*place, 0)[...].astype(jnp.float32)
        for dk in range(1, k_count):
            value = value + landed(("k", *place, dk))
        return value

    index_of = {}

    def keep(place, value):
        index_of[place] = len(index_of)
        sums[index_of[place]] = value.astype(jnp.bfloat16)
        return index_of[place]

    def mix_core(dx):
        value = head_ref[mix_span(dx, 0), :].astype(jnp.float32)
        for dk in range(1, k_count):
            value = value + landed(("mk", dx, dk))
        return value

    def finish(dz, dy):
        if dy:
            for dx in range(1, x_count):
                index = keep((dz, dy, dx), core_sum((dz, dy, dx)))
                send(("p", dz, dy, dx), sums.at[index, pl.ds(0, half_rows)], dy=dy)
                send(("q", dz, dy, dx), sums.at[index, pl.ds(half_rows, half_rows)], dx=dx)
            return
        for over in range(1, y_count):
            value = core_sum((dz, over, 0))
            upper, lower = value[:half_rows], value[half_rows:]
            for dx in range(1, x_count):
                lower = lower + landed(("q", dz, over, dx))
            index = keep((dz, over, 0), jnp.concatenate([upper, lower], 0))
            send(("y", dz, over), sums.at[index], dy=over)
        for dx in range(1, x_count):
            value = core_sum((dz, 0, dx))
            upper, lower = value[:half_rows], value[half_rows:]
            for over in range(1, y_count):
                upper = upper + landed(("p", dz, over, dx))
            index = keep((dz, 0, dx), jnp.concatenate([upper, lower], 0))
            send(("x", dz, dx), sums.at[index], dx=dx)

    blocks = [(dz, dy) for dy in list(range(1, y_count)) + [0] for dz in z_steps]
    for turn, block in enumerate(blocks):
        compute(*block)
        if turn:
            finish(*blocks[turn - 1])
        else:
            for dx in range(1, x_count):
                mix_sums[dx - 1] = mix_core(dx).astype(jnp.bfloat16)
                send(("mx", dx), mix_sums.at[dx - 1], dx=dx)
    finish(*blocks[-1])
    mixture = mix_core(0)
    for dx in range(1, x_count):
        mixture = mixture + landed(("mx", dx))
    scale = lax.rsqrt(jnp.mean(mixture * mixture, -1, keepdims=True) + EPS)
    mixed_ref[...] = (mixture * scale * gain_ref[...]).astype(jnp.bfloat16)
    for dz in z_steps:
        value = core_sum((dz, 0, 0))
        for dx in range(1, x_count):
            value = value + landed(("x", dz, dx))
        for dy in range(1, y_count):
            value = value + landed(("y", dz, dy))
        if dz:
            index = keep((dz, 0, 0), value)
            send(("z", dz), sums.at[index], dz=dz)
    for dz in range(1, z_count):
        value = value + landed(("z", dz))
    out_ref[...] = value.astype(jnp.bfloat16)
    for copy in sent:
        copy.wait_send()


def reduce_all(expert_args, head_part, gain, ep_count, tp_count):
    dims = grid_of(ep_count, tp_count)
    _, sizes = reduce_slots(dims)
    count, model_width = expert_args[0].shape
    rows = count // ep_count
    width = model_width // tp_count
    mix_rows = head_part.shape[0] // tp_count
    mix_width = head_part.shape[1]
    vmem = pl.BlockSpec(memory_space=pltpu.VMEM)
    semaphores = pltpu.SemaphoreType.DMA((len(reduce_keys(dims)),))
    return pl.pallas_call(
        functools.partial(reduce_kernel, dims),
        out_shape=[
            jax.ShapeDtypeStruct((mix_rows, mix_width), jnp.bfloat16),
            jax.ShapeDtypeStruct((rows, width), jnp.bfloat16),
        ],
        in_specs=[vmem] * (len(expert_args) + 2),
        out_specs=[vmem] * 2,
        scratch_shapes=[
            pltpu.VMEM((ep_count, tp_count, rows, width), jnp.bfloat16),
            pltpu.VMEM((sizes["full"], rows, width), jnp.bfloat16),
            pltpu.VMEM((sizes["pq"], rows // 2, width), jnp.bfloat16),
            pltpu.VMEM((sizes["m"], mix_rows, mix_width), jnp.bfloat16),
            pltpu.VMEM((dims[0] * dims[1] * dims[2], rows, width), jnp.bfloat16),
            pltpu.VMEM((max(1, dims[2] - 1), mix_rows, mix_width), jnp.bfloat16),
            semaphores,
            semaphores,
        ],
        compiler_params=pltpu.CompilerParams(
            collective_id=1, has_side_effects=True, vmem_limit_bytes=48 * 1024 * 1024
        ),
    )(*expert_args, head_part, gain)


def per_device_dense(
    query_latent,
    keyval_latent,
    rotary_key,
    query_gain,
    keyval_gain,
    query_weight,
    keyval_weight,
    output_weight,
    output_gain,
    second_rows,
    second_gain,
    route_ids,
    route_weights,
    gate_weight,
    up_weight,
    down_weight,
    shared_gate,
    shared_up,
    shared_down,
):
    first_rows = query_latent.shape[0]
    tp_count = lax.axis_size("tp")
    ep_count = lax.axis_size("ep")
    head_count = query_weight.shape[1] // (NOPE + ROPE)
    start_row = lax.axis_index("ep") * first_rows
    quarter = first_rows // tp_count
    offset = lax.axis_index("tp") * quarter
    second_quarter = second_rows.shape[0] // tp_count
    second_offset = lax.axis_index("tp") * second_quarter

    own_latent = rms_scale(
        lax.dynamic_slice_in_dim(keyval_latent, offset, quarter, 0), keyval_gain
    )
    own_positions = (start_row + offset).astype(jnp.float32) + jnp.arange(
        quarter, dtype=jnp.float32
    )
    own_rot = rotate(
        lax.dynamic_slice_in_dim(rotary_key, offset, quarter, 0).astype(jnp.float32),
        own_positions,
    ).astype(jnp.bfloat16)
    ids = lax.dynamic_slice_in_dim(route_ids, second_offset, second_quarter, 0)
    wts = lax.dynamic_slice_in_dim(route_weights, second_offset, second_quarter, 0)
    dense = jnp.sum(
        jnp.where(
            ids[:, :, None] == jnp.arange(ep_count, dtype=jnp.int32)[None, None, :],
            wts[:, :, None],
            0.0,
        ),
        1,
    )
    dense_high = dense.astype(jnp.bfloat16)
    dense_low = (dense - dense_high.astype(jnp.float32)).astype(jnp.bfloat16)
    latent_width = own_latent.shape[1]
    used = latent_width + ROPE + 2 * ep_count
    fill = -used % 128
    packed = jnp.concatenate(
        [own_latent, own_rot, dense_high, dense_low, jnp.zeros((quarter, fill), jnp.bfloat16)], 1
    )
    own_normed = rms_scale(
        lax.dynamic_slice_in_dim(second_rows, second_offset, second_quarter, 0), second_gain
    )
    packed, normed = gather_all([packed, own_normed], ep_count, tp_count)

    positions = start_row.astype(jnp.float32) + jnp.arange(first_rows, dtype=jnp.float32)
    queries = jnp.dot(
        rms_scale(query_latent, query_gain), query_weight, preferred_element_type=jnp.float32
    ).reshape(first_rows, head_count, NOPE + ROPE)
    queries = jnp.concatenate(
        [queries[..., :NOPE], rotate(queries[..., NOPE:], positions)], -1
    ).astype(jnp.bfloat16)
    all_latent = packed[:, :latent_width]
    all_rot = packed[:, latent_width : latent_width + ROPE]
    total_keys = packed.shape[0]
    keyvals = (
        jnp.dot(all_latent, keyval_weight, preferred_element_type=jnp.float32)
        .astype(jnp.bfloat16)
        .reshape(total_keys, head_count, NOPE + VDIM)
    )
    keys = jnp.concatenate(
        [
            keyvals[..., :NOPE],
            jnp.broadcast_to(all_rot[:, None, :], (total_keys, head_count, ROPE)),
        ],
        -1,
    )
    scores = jnp.einsum("qhd,khd->hqk", queries, keys, preferred_element_type=jnp.float32) * (
        (NOPE + ROPE) ** (-0.5)
    )
    exponent = jnp.exp(scores - jnp.max(scores, -1, keepdims=True))
    denominator = jnp.sum(exponent, -1)
    accumulated = jnp.einsum(
        "hqk,khe->qhe",
        exponent.astype(jnp.bfloat16),
        keyvals[..., NOPE:],
        preferred_element_type=jnp.float32,
    )
    attended = (
        (accumulated / denominator.T[..., None])
        .astype(jnp.bfloat16)
        .reshape(first_rows, head_count * VDIM)
    )
    head_part = jnp.dot(attended, output_weight, preferred_element_type=jnp.float32).astype(
        jnp.bfloat16
    )

    me = lax.axis_index("ep")
    high = lax.dynamic_slice_in_dim(packed, latent_width + ROPE + me, 1, 1)
    low = lax.dynamic_slice_in_dim(packed, latent_width + ROPE + ep_count + me, 1, 1)
    scale = high.astype(jnp.float32) + low.astype(jnp.float32)
    expert_args = (
        normed,
        scale,
        gate_weight[0],
        up_weight[0],
        down_weight[0],
        shared_gate,
        shared_up,
        shared_down,
    )
    mixed, expert_mix = reduce_all(
        expert_args, head_part, output_gain.reshape(1, -1), ep_count, tp_count
    )
    return (mixed, expert_mix)


def solution(mesh):
    placed = (
        P("ep", None),
        P("ep", None),
        P("ep", None),
        P(),
        P(),
        P(None, "tp"),
        P(None, "tp"),
        P("tp", None),
        P(),
        P("ep", None),
        P(),
        P("ep", None),
        P("ep", None),
        P("ep", None, "tp"),
        P("ep", None, "tp"),
        P("ep", "tp", None),
        P(None, "tp"),
        P(None, "tp"),
        P("tp", None),
    )
    def per_device(*args):
        tok_rows, top_count = args[11].shape
        expert_count = args[13].shape[0] * mesh.shape["ep"]
        capacity = tok_rows * top_count * 2 // expert_count
        if args[13].shape[0] == 1 and capacity >= tok_rows:
            return per_device_dense(*args)
        return per_device_slots(*args)

    return jax.shard_map(
        per_device,
        mesh=mesh,
        in_specs=placed,
        out_specs=(P(("ep", "tp"), None), P("ep", "tp")),
        check_vma=False,
    )
```
